32 devices in a mesh: sp: 8 (over z, x), tp: 4 (over y, core).
Axes of the slice: x: 2, y: 2, z: 4, core: 2. Of those that a mesh axis runs over, the one named last changes fastest.
Arguments:
- expert_input: bfloat16 [1536, 2048], P('sp'), may hold values from -6 to 6
- norm_gain: float32 [2048], replicated, may hold values from 0.1 to 1.9
- expert_ids: int32 [1536, 2], P('sp'), may hold values from 0 to 7, all different within a row; in each aligned block of 192 rows (0 to 191, 192 to 383, ...) at most 96 rows name the same one
- route_weights: float32 [1536, 2], P('sp'), may hold values from 0.25 to 2.25
- layer_cotangent: bfloat16 [1536, 2048], P('sp'), may hold values from -6 to 6
- gate_weight: bfloat16 [8, 1024, 2048], P('sp', 'tp'), may hold values from -0.125 to 0.125
- up_weight: bfloat16 [8, 1024, 2048], P('sp', 'tp'), may hold values from -0.125 to 0.125
- down_weight: bfloat16 [8, 1024, 2048], P('sp', 'tp'), may hold values from -0.1875 to 0.1875
- proj_b: bfloat16 [1536, 2048], P('sp', 'tp'), may hold values from -6 to 6
- proj_c: bfloat16 [1536, 2048], P('sp', 'tp'), may hold values from -6 to 6
- proj_x: bfloat16 [1536, 2048], P('sp', 'tp'), may hold values from -6 to 6
- conv_taps: float32 [3, 2048], P(None, 'tp'), may hold values from -3 to 3
- out_weight: bfloat16 [2048, 2048], P(None, 'tp'), may hold values from -0.125 to 0.125
Outputs:
- grad_gate: bfloat16 [8, 1024, 2048], P('sp', 'tp')
- grad_up: bfloat16 [8, 1024, 2048], P('sp', 'tp')
- grad_down: bfloat16 [8, 1024, 2048], P('sp', 'tp')
- grad_out_weight: float32 [2048, 2048], P('sp', 'tp')
- grad_b: bfloat16 [1536, 2048], P('sp', 'tp')
- grad_c: bfloat16 [1536, 2048], P('sp', 'tp')
- grad_x: bfloat16 [1536, 2048], P('sp', 'tp')
The draws below stay inside these ranges and needn't reach their ends.
Inputs may be any that keep to these rules, and one draw needn't show every extreme that they name: `expert_ids`: A token's two experts differ. In the rows of one device each expert is named at most 96 times, a bound that some expert reaches in some blocks.
All inputs are finite; a program needn't handle non-finite values.
Results may differ from the reference program's by a relative error of at most 0.034.
Values may be sent and summed in bfloat16 or wider, within the bound.
A program may use at most 64 MiB of HBM per device.

```python
import math
import jax
import jax.numpy as jnp
import numpy as np
from jax import lax

D = 2048
FF = 1024
W_A = 2048
TOK_DEV = 192
TOKENS = 1536
EXPERTS = 8
CAP = 96
N_SP = 8
N_TP = 4


def raised(drawn, own_key, source, target, shards_of, factor):
    def block_of(position):
        return (jnp.arange(drawn.shape[position]) // (drawn.shape[position] // shards_of)).reshape((-1,) + (1,) * (drawn.ndim - 1 - position))

    near = jax.random.permutation(own_key, shards_of)[block_of(target)]
    other_side = (block_of(target) + shards_of // 2) % shards_of
    return jnp.where((block_of(source) == near) | (block_of(source) == other_side), factor * drawn, drawn)


def block_levels(own_key, extent, cuts, least, high):
    level, own = 1.0, jax.random.fold_in(own_key, 6)
    for axis_at, shards_of in cuts:
        steps = jnp.exp(jax.random.uniform(jax.random.fold_in(own, axis_at), (shards_of,), jnp.float32, least / len(cuts), high / len(cuts)))
        level = level * jnp.repeat(steps, extent[axis_at] // shards_of).reshape([-1 if axis == axis_at else 1 for axis in range(len(extent))])
    return level


def deal_out(key, own, number, rows, number_of, top, bound, skew):
    ranking = jax.random.permutation(key, number_of)
    heavy_load, ordinary = shares(number_of, rows * top, bound, skew, True), shares(number_of, rows * top, bound, skew, False)
    places = jnp.arange(number_of)

    def named(lengths, rotation):
        used = int((lengths > 0).sum())
        fixed = max(1, used // 4)
        shifted = fixed + (places - fixed + rotation * (used - fixed)) % max(1, number_of - fixed)
        return jnp.zeros((number_of,), jnp.int32).at[ranking[jnp.where(places < fixed, places, shifted)]].set(jnp.asarray(lengths, jnp.int32))

    lengths = jnp.where(number % 4 == 0, named(heavy_load, number // 4), named(ordinary, number - number // 4 - 1))
    mixed = jax.random.permutation(jax.random.fold_in(own, 3), number_of)
    source_of, taker = mixed[0:number_of // 2 * 2:2], mixed[1:number_of // 2 * 2:2]
    margin = jnp.minimum(lengths[source_of] - 1, bound - lengths[taker]) // 2
    margin = jnp.where((source_of == ranking[0]) | (taker == ranking[0]) | (lengths[taker] == 0), 0, jnp.maximum(margin, 0))
    shifted = jax.random.randint(jax.random.fold_in(own, 4), (number_of // 2,), 0, 1 << 20) % (margin + 1)
    lengths = lengths.at[source_of].add(-shifted).at[taker].add(shifted)
    members = jnp.searchsorted(jnp.cumsum(lengths), jnp.arange(rows * top), side="right").astype(jnp.int32)
    table = members.reshape(top, rows).T
    table = table[jax.random.permutation(jax.random.fold_in(own, 1), rows)]
    rotation = jax.random.randint(jax.random.fold_in(own, 2), (rows, 1), 0, top)
    return jnp.take_along_axis(table, (jnp.arange(top)[None, :] + rotation) % top, axis=1)


def shares(amount, total, limit, slope, full):
    weights = [(1 << 20) // math.isqrt(standing ** slope) + 1 for standing in range(1, amount + 1)]
    largest = limit if full else min(limit, max(-(-total // amount), total * weights[0] // sum(weights)))
    least = 1 if total - largest >= amount - 1 else 0
    holding, rest = [largest] + [least] * (amount - 1), total - largest - least * (amount - 1)
    while rest > 0:
        free = [i for i in range(1, amount) if holding[i] < largest] or [i for i in range(1, amount) if holding[i] < limit]
        pool, budget = sum([weights[i] for i in free]), rest
        for i in free:
            extra = min(limit - holding[i], max(1, budget * weights[i] // pool), rest)
            holding[i] = holding[i] + extra
            rest = rest - extra
    return np.array(holding)


def scatter_about(key, extent, width, reach, shards=(), held_as=jnp.bfloat16):
    entries = jax.random.normal(key, extent, jnp.float32) * width
    if len(shards) > 0:
        entries = block_levels(key, extent, shards, -0.22, 0.18) * entries
    return jnp.clip(entries, min=-reach, max=reach).astype(held_as)


def noise_with(key, dims, deviation, most, pieces, heavy, kind=jnp.bfloat16):
    values = deviation * jax.random.normal(key, dims, jnp.float32)
    if pieces:
        values = values * block_levels(key, dims, pieces, -0.22, 0.18)
    return jnp.clip(raised(values, jax.random.fold_in(key, 3), *heavy), -most, most).astype(kind)


def setup_inputs(seed: int = 0) -> dict:
    splits = jax.random.split(jax.random.key(seed), 14)
    expert_input = scatter_about(splits[0], (TOKENS, D), 1.0, 6.0, ((0, 8),))
    norm_gain = jnp.clip(1.0 + 0.18 * jax.random.normal(splits[1], (D,), jnp.float32), 0.1, 1.9)
    expert_ids_keys = jax.random.split(jax.random.fold_in(splits[2], 1), TOKENS // TOK_DEV)
    expert_ids_turns = jax.random.permutation(jax.random.fold_in(splits[2], 3), TOKENS // TOK_DEV)
    expert_ids = jax.vmap(lambda own, number: deal_out(jax.random.fold_in(splits[2], 2), own, number, TOK_DEV, EXPERTS, 2, CAP, 2))(expert_ids_keys, expert_ids_turns).reshape((TOKENS, 2))
    route_weights = jnp.clip(0.25 + 2.0 * jax.random.uniform(splits[3], (TOKENS, 2), jnp.float32) ** block_levels(splits[3], (TOKENS, 2), ((0, 8),), -0.2, 0.2), 0.25, 2.25)
    layer_cotangent = noise_with(splits[4], (TOKENS, D), 1.0, 6.0, ((0, 8),), (0, 1, 8, 2.0))
    gate_weight = scatter_about(splits[5], (EXPERTS, FF, D), D ** -0.5, 0.125, ((0, 8), (1, 4)))
    up_weight = scatter_about(splits[6], (EXPERTS, FF, D), D ** -0.5, 0.125, ((0, 8), (1, 4)))
    down_weight = scatter_about(splits[7], (EXPERTS, FF, D), FF ** -0.5, 0.1875, ((0, 8), (1, 4)))
    proj_b = scatter_about(splits[8], (TOKENS, W_A), 1.0, 6.0, ((0, 8), (1, 4)))
    proj_c = scatter_about(splits[9], (TOKENS, W_A), 1.0, 6.0, ((0, 8), (1, 4)))
    proj_x = scatter_about(splits[10], (TOKENS, W_A), 1.0, 6.0, ((0, 8), (1, 4)))
    conv_taps = scatter_about(splits[11], (3, W_A), 0.58, 3.0, ((1, 4),), jnp.float32)
    out_weight = scatter_about(splits[12], (D, W_A), W_A ** -0.5, 0.125, ((1, 4),))
    return {"expert_input": expert_input, "norm_gain": norm_gain, "expert_ids": expert_ids, "route_weights": route_weights, "layer_cotangent": layer_cotangent, "gate_weight": gate_weight, "up_weight": up_weight, "down_weight": down_weight, "proj_b": proj_b, "proj_c": proj_c, "proj_x": proj_x, "conv_taps": conv_taps, "out_weight": out_weight}


eps = 1e-06

def slot_layout(routed_block):
    pair_count = routed_block.shape[0]
    onehot = (routed_block[:, None] == jnp.arange(EXPERTS, dtype=jnp.int32)[None, :]).astype(jnp.int32)
    slot_rank = lax.optimization_barrier(jnp.sum((jnp.cumsum(onehot, axis=0) - 1) * onehot, axis=1))
    slot_index = (routed_block * CAP + slot_rank).astype(jnp.int32)
    pair_of = jnp.zeros((EXPERTS * CAP,), jnp.int32).at[slot_index].set(jnp.arange(pair_count, dtype=jnp.int32))
    filled = jnp.zeros((EXPERTS * CAP,), jnp.int32).at[slot_index].set(1)
    return (slot_index, pair_of, filled)

def build_block(routed_block, normed_block, cot_block, weight_block):
    slot_index, pair_of, filled = slot_layout(routed_block)
    token_of = pair_of // 2
    filled_mask = (filled > 0)[:, None]
    rows = jnp.where(filled_mask, normed_block[token_of], jnp.zeros((), jnp.bfloat16))
    scaled = weight_block[pair_of][:, None] * cot_block[token_of].astype(jnp.float32)
    cots = jnp.where(filled_mask, scaled, 0.0).astype(jnp.bfloat16)
    return (rows.reshape(EXPERTS, CAP, D), cots.reshape(EXPERTS, CAP, D), slot_index)

def expert_grads(operands):
    rows, cots, w_gate, w_up, w_down = operands
    row_count = rows.shape[0]
    gate_pre = jnp.dot(rows, w_gate.T, preferred_element_type=jnp.float32)
    up_pre = jnp.dot(rows, w_up.T, preferred_element_type=jnp.float32)
    grad_hidden = jnp.dot(cots, w_down.T, preferred_element_type=jnp.float32)
    sigmoid_gate = jax.nn.sigmoid(gate_pre)
    hidden = (gate_pre * sigmoid_gate * up_pre).astype(jnp.bfloat16)
    down_grad = jnp.dot(hidden.T, cots, preferred_element_type=jnp.float32).astype(jnp.bfloat16)
    grad_gate_pre = (grad_hidden * up_pre * sigmoid_gate * (1.0 + gate_pre * (1.0 - sigmoid_gate))).astype(jnp.bfloat16)
    grad_up_pre = (grad_hidden * gate_pre * sigmoid_gate).astype(jnp.bfloat16)
    gate_grad = jnp.dot(grad_gate_pre.T, rows, preferred_element_type=jnp.float32).astype(jnp.bfloat16)
    up_grad = jnp.dot(grad_up_pre.T, rows, preferred_element_type=jnp.float32).astype(jnp.bfloat16)
    block_width = FF // N_TP
    partial_value = jnp.einsum('rtf,tfd->rtd', grad_gate_pre.astype(jnp.float32).reshape(row_count, N_TP, block_width), w_gate.astype(jnp.float32).reshape(N_TP, block_width, D))
    partial_value = partial_value + jnp.einsum('rtf,tfd->rtd', grad_up_pre.astype(jnp.float32).reshape(row_count, N_TP, block_width), w_up.astype(jnp.float32).reshape(N_TP, block_width, D))
    rounded = lax.optimization_barrier(partial_value.astype(jnp.bfloat16)).astype(jnp.float32)
    input_grad = lax.optimization_barrier(jnp.sum(rounded, axis=1)).astype(jnp.bfloat16)
    return (gate_grad, up_grad, down_grad, input_grad)

def reference(expert_input, norm_gain, expert_ids, route_weights, layer_cotangent, gate_weight, up_weight, down_weight, proj_b, proj_c, proj_x, conv_taps, out_weight):
    layer_in = expert_input.astype(jnp.float32)
    root_mean = jnp.sqrt(lax.optimization_barrier(jnp.mean(layer_in * layer_in, axis=1, keepdims=True)) + eps)
    unit = layer_in / root_mean
    normed = (unit * norm_gain[None, :]).astype(jnp.bfloat16)
    routed_blocks = expert_ids.reshape(N_SP, TOK_DEV * 2).astype(jnp.int32)
    weight_blocks = route_weights.reshape(N_SP, TOK_DEV * 2)
    rows_all, cots_all, slots_all = jax.vmap(build_block)(routed_blocks, normed.reshape(N_SP, TOK_DEV, D), layer_cotangent.reshape(N_SP, TOK_DEV, D), weight_blocks)
    rows_expert = jnp.swapaxes(rows_all, 0, 1).reshape(EXPERTS, N_SP * CAP, D)
    cots_expert = jnp.swapaxes(cots_all, 0, 1).reshape(EXPERTS, N_SP * CAP, D)
    gate_grad, up_grad, down_grad, input_grad = lax.map(expert_grads, (rows_expert, cots_expert, gate_weight, up_weight, down_weight))
    back_blocks = jnp.swapaxes(input_grad.reshape(EXPERTS, N_SP, CAP, D), 0, 1).reshape(N_SP, EXPERTS * CAP, D)

    def collect(back_block, slot_index):
        pairs_grad = back_block[slot_index].astype(jnp.float32)
        return pairs_grad.reshape(TOK_DEV, 2, D).sum(axis=1)
    grad_normed = jax.vmap(collect)(back_blocks, slots_all).reshape(TOKENS, D)
    row_total = lax.optimization_barrier(jnp.sum(unit * norm_gain[None, :] * grad_normed, axis=1, keepdims=True))
    grad_input = (layer_cotangent.astype(jnp.float32) + (norm_gain[None, :] * grad_normed - unit * row_total / D) / root_mean).astype(jnp.bfloat16)
    product = proj_c.astype(jnp.float32) * proj_x.astype(jnp.float32)
    padded = jnp.pad(product, ((2, 0), (0, 0)))
    conv = conv_taps[0][None, :] * padded[:-2] + conv_taps[1][None, :] * padded[1:-1] + conv_taps[2][None, :] * padded[2:]
    mixed = (proj_b.astype(jnp.float32) * conv).astype(jnp.bfloat16)
    grad_out_weight = jnp.dot(grad_input.T, mixed, preferred_element_type=jnp.float32)
    grad_mixed = jnp.dot(grad_input, out_weight, preferred_element_type=jnp.float32).astype(jnp.bfloat16)
    grad_b = (grad_mixed.astype(jnp.float32) * conv).astype(jnp.bfloat16)
    grad_conv = grad_mixed.astype(jnp.float32) * proj_b.astype(jnp.float32)
    padded_back = jnp.pad(grad_conv, ((0, 2), (0, 0)))
    grad_product = conv_taps[2][None, :] * padded_back[:-2] + conv_taps[1][None, :] * padded_back[1:-1] + conv_taps[0][None, :] * padded_back[2:]
    grad_c = (grad_product * proj_x.astype(jnp.float32)).astype(jnp.bfloat16)
    grad_x = (grad_product * proj_c.astype(jnp.float32)).astype(jnp.bfloat16)
    return (gate_grad, up_grad, down_grad, grad_out_weight, grad_b, grad_c, grad_x)
```

```python
import functools

import jax
import jax.numpy as jnp
from jax import lax
from jax.experimental import pallas as pl
from jax.experimental.pallas import tpu as pltpu
from jax.sharding import PartitionSpec as P

eps = 1e-06
MESH = pl.DeviceIdType.MESH
f32 = jnp.float32
bf16 = jnp.bfloat16

NT = (((1,), (1,)), ((), ()))
TN = (((0,), (0,)), ((), ()))


def dot(a, b, dims=(((1,), (0,)), ((), ()))):
    return lax.dot_general(a, b, dims, preferred_element_type=f32)


def kernel(
    dims,
    x_ref, gain_ref, ids_ref, rw_ref, cot_ref, wg_h, wu_h, wd_h, pb_ref, pc_ref, px_ref, taps_ref, ow_h,
    gg_h, gu_h, gd_h, gow_ref, gb_ref, gc_ref, gx_ref,
    wg, wu, wd, ow, perm, send, R, hid, ggp, gup, pown, pcs, pcr, ysnd, yrcv, bsnd, back,
    gn, gi, GI, MX, conv, gmix, halo_s, halo_r, tail_s, tail_r, ggv, guv, gdv,
    lsem, osem, own_sem, a_s, r_sem, f_s, f2_s, p_s, p_r, y_s, y_r, b_s, b_r,
    n_s, n_r, n2_s, m_s, m_r, m2_s, g_s, g_r, g2_s, g2_r, h_s, h_r,
):
    G, T, C, lo = dims
    Y = T // 2
    H = G // lo
    tok, D = x_ref.shape
    col = D // T
    DB = D // G
    half = tok // 2
    me = lax.axis_index("sp")
    tp = lax.axis_index("tp")
    y = tp // 2
    c = lax.rem(tp, 2)
    oc = 1 - c
    ptn = y * 2 + oc

    def ring(v):
        return lax.rem(v + G, G)

    def yk(k):
        return lax.rem(y + k, Y)

    def rc(src, dst, ss, rs, sp, t):
        return pltpu.make_async_remote_copy(
            src_ref=src, dst_ref=dst, send_sem=ss, recv_sem=rs,
            device_id={"sp": sp, "tp": t}, device_id_type=MESH,
        )

    def far(i):
        k = i - 1
        d = G // 2 + ((k + 1) // 2) * (1 - 2 * lax.rem(k + 2, 2))
        return jnp.where(i == 0, 0, d)

    def src_at(i):
        return ring(me - far(i))

    def dst_at(i):
        return ring(me + far(i))

    loads = [
        pltpu.make_async_copy(h, v, lsem.at[n])
        for n, (h, v) in enumerate(((wg_h, wg), (wu_h, wu), (wd_h, wd), (ow_h, ow)))
    ]
    for ld in loads:
        ld.start()

    barrier = pltpu.get_barrier_semaphore()

    def greet(d, _):
        pl.semaphore_signal(barrier, inc=1, device_id={"sp": ring(me + d), "tp": tp}, device_id_type=MESH)
        return 0

    lax.fori_loop(1, G, greet, 0)
    for k in range(1, Y):
        pl.semaphore_signal(barrier, inc=1, device_id={"sp": me, "tp": yk(k) * 2 + c}, device_id_type=MESH)
    pl.semaphore_signal(barrier, inc=1, device_id={"sp": me, "tp": ptn}, device_id_type=MESH)

    xf = x_ref[...].astype(f32)
    rm = jnp.sqrt(jnp.mean(xf * xf, axis=1, keepdims=True) + eps)
    my_cols = pl.ds(pl.multiple_of(tp * col, col), col)
    ncols = ((x_ref[:, my_cols].astype(f32) / rm) * gain_ref[:, my_cols]).astype(bf16)
    ids = ids_ref[...]
    expert = lax.broadcasted_iota(jnp.int32, (G, tok), 0)
    is0 = expert == ids[0:1]
    is1 = expert == ids[1:2]
    both = jnp.where(is0 | is1, 1.0, 0.0).astype(bf16)
    earlier = jnp.where(
        lax.broadcasted_iota(jnp.int32, (tok, tok), 0) < lax.broadcasted_iota(jnp.int32, (tok, tok), 1), 1.0, 0.0
    ).astype(bf16)
    rank = dot(both, earlier)
    slot0 = jnp.sum(jnp.where(is0, rank, 0.0), axis=0, keepdims=True) + ids[0:1].astype(f32) * C
    slot1 = jnp.sum(jnp.where(is1, rank, 0.0), axis=0, keepdims=True) + ids[1:2].astype(f32) * C
    place = lax.broadcasted_iota(jnp.int32, (G * C, tok), 0).astype(f32)
    at0 = place == slot0
    at1 = place == slot1
    perm[...] = jnp.where(at0 | at1, 1.0, 0.0).astype(bf16)
    wslot = jnp.sum(jnp.where(at0, rw_ref[0:1], 0.0) + jnp.where(at1, rw_ref[1:2], 0.0), axis=1, keepdims=True)
    send[:, 0] = dot(perm[...], ncols).astype(bf16).reshape(G, C, col)
    send[:, 1] = (dot(perm[...], cot_ref[:, my_cols]) * wslot).astype(bf16).reshape(G, C, col)

    halo_s[...] = pc_ref[tok - 8:, :].astype(f32) * px_ref[tok - 8:, :].astype(f32)

    pl.semaphore_wait(barrier, G - 1 + Y)

    halo = rc(halo_s, halo_r, h_s.at[0], h_r.at[0], ring(me + 1), tp)
    halo.start()
    own = pltpu.make_async_copy(send.at[me], R.at[tp, me], own_sem)
    own.start()

    def a_copy(i):
        e = dst_at(i)
        return rc(send.at[e], R.at[tp, me], a_s.at[e], r_sem.at[tp, me], e, tp)

    def issue_a(i, _):
        a_copy(i).start()
        return 0

    lax.fori_loop(1, G, issue_a, 0)

    product = pc_ref[...].astype(f32) * px_ref[...].astype(f32)
    halo.wait_recv()
    before = jnp.where(me > 0, halo_r[...], 0.0)
    padded = jnp.concatenate([before, product], axis=0)
    cv = taps_ref[0:1] * padded[6:6 + tok] + taps_ref[1:2] * padded[7:7 + tok] + taps_ref[2:3] * product
    conv[...] = cv
    MX[me] = (pb_ref[...].astype(f32) * cv).astype(bf16)
    hi, low = me // lo, lax.rem(me, lo)

    def m_copy(d):
        h2 = lax.rem(hi + d, H)
        return rc(MX.at[me], MX.at[me], m_s.at[h2], m_r.at[me], h2 * lo + low, tp)

    for ld in loads[:3]:
        ld.wait()
    own.wait()

    def r_wait(j, s):
        rc(R.at[j, s], R.at[j, s], own_sem, r_sem.at[j, s], me, ptn).wait_recv()

    def fwd(n, s):
        t = ptn if n == 0 else yk(n) * 2 + c
        return rc(R.at[tp, s], R.at[tp, s], f_s.at[n, s], r_sem.at[tp, s], me, t)

    def fwd2(k, s):
        j = yk(k) * 2 + c
        return rc(R.at[j, s], R.at[j, s], f2_s.at[k, s], r_sem.at[j, s], me, ptn)

    def p_copy(s):
        return rc(pcs.at[s], pcr.at[s], p_s.at[s], p_r.at[s], me, ptn)

    def y_copy(k, s):
        yo = yk(k)
        return rc(ysnd.at[s, yo], yrcv.at[s, y], y_s.at[yo, s], y_r.at[y, s], me, yo * 2 + c)

    def b_copy(s):
        return rc(bsnd.at[s], back.at[me], b_s.at[s], b_r.at[me], s, tp)

    def cols(j):
        return pl.ds(pl.multiple_of(j * col, col), col)

    def step(i, _):
        @pl.when(i < G)
        def _():
            s = src_at(i)

            @pl.when(i > 0)
            def _():
                r_wait(tp, s)

            for n in range(Y - 1, -1, -1):
                fwd(n, s).start()

        @pl.when((i >= 1) & (i < G + 1))
        def _():
            s = src_at(i - 1)
            for k in range(1, Y):
                r_wait(yk(k) * 2 + c, s)
                fwd2(k, s).start()

        @pl.when((i >= 2) & (i < G + 2))
        def _():
            s = src_at(i - 2)
            for yy in range(Y):
                r_wait(yy * 2 + oc, s)
            gate = jnp.zeros((C, wg.shape[0]), f32)
            up = gate
            gh = gate
            for j in range(T):
                rows = R[j, s, 0]
                cots = R[j, s, 1]
                cs = slice(j * col, (j + 1) * col)
                gate = gate + dot(rows, wg[:, cs], NT)
                up = up + dot(rows, wu[:, cs], NT)
                gh = gh + dot(cots, wd[:, cs], NT)
            sg = jax.nn.sigmoid(gate)
            hid[s] = (gate * sg * up).astype(bf16)
            a = (gh * up * sg * (1.0 + gate * (1.0 - sg))).astype(bf16)
            b = (gh * gate * sg).astype(bf16)
            ggp[s] = a
            gup[s] = b
            for yy in range(Y):
                jo = cols(yy * 2 + oc)
                pcs[s, yy] = (dot(a, wg[:, jo]) + dot(b, wu[:, jo])).astype(bf16)
            p_copy(s).start()
            for yy in range(Y):
                jm = cols(yy * 2 + c)
                pown[s, yy] = dot(a, wg[:, jm]) + dot(b, wu[:, jm])

        @pl.when((i >= 3) & (i < G + 3))
        def _():
            s = src_at(i - 3)
            p_copy(s).wait_recv()
            for k in range(1, Y):
                yo = yk(k)
                ysnd[s, yo] = (pown[s, yo] + pcr[s, yo].astype(f32)).astype(bf16)
                y_copy(k, s).start()

        @pl.when(i >= 4)
        def _():
            s = src_at(i - 4)
            total = pown[s, y] + pcr[s, y].astype(f32)
            for k in range(1, Y):
                yo = yk(k)
                rc(ysnd.at[s, yo], yrcv.at[s, yo], y_s.at[yo, s], y_r.at[yo, s], me, yo * 2 + c).wait_recv()
                total = total + yrcv[s, yo].astype(f32)

            @pl.when(i > 4)
            def _():
                bsnd[s] = total.astype(bf16)
                b_copy(s).start()

            @pl.when(i == 4)
            def _():
                back[me] = total.astype(bf16)

        return 0

    lax.fori_loop(0, G + 4, step, 0)

    for d in range(1, H):
        m_copy(d).start()

    def m2_copy(d, h2):
        lw = lax.rem(low + d, lo)
        s = h2 * lo + low
        return rc(MX.at[s], MX.at[s], m2_s.at[d, h2], m_r.at[s], hi * lo + lw, tp)

    for d in range(1, lo):
        m2_copy(d, hi).start()

    def wgrad(j, _):
        rows = R[j, :, 0].reshape(G * C, col)
        cots = R[j, :, 1].reshape(G * C, col)
        F = wg.shape[0]
        gdv[:, cols(j)] = dot(hid[...].reshape(G * C, F), cots, TN).astype(bf16)
        ggv[:, cols(j)] = dot(ggp[...].reshape(G * C, F), rows, TN).astype(bf16)
        guv[:, cols(j)] = dot(gup[...].reshape(G * C, F), rows, TN).astype(bf16)
        return 0

    lax.fori_loop(0, T, wgrad, 0)
    outs = [
        pltpu.make_async_copy(v, h, osem.at[n]) for n, (v, h) in enumerate(((ggv, gg_h), (guv, gu_h), (gdv, gd_h)))
    ]
    for o in outs:
        o.start()

    def back_wait(i, _):
        s = src_at(i)
        rc(back.at[s], back.at[s], b_s.at[s], b_r.at[s], s, tp).wait_recv()
        return 0

    lax.fori_loop(1, G, back_wait, 0)
    gn[tp] = dot(perm[...], back[...].reshape(G * C, col), TN).astype(bf16)

    def n_copy(n):
        t = ptn if n == 0 else yk(n) * 2 + c
        return rc(gn.at[tp], gn.at[tp], n_s.at[n], n_r.at[tp], me, t)

    def n2_copy(k):
        j = yk(k) * 2 + c
        return rc(gn.at[j], gn.at[j], n2_s.at[k], n_r.at[j], me, ptn)

    for n in range(Y - 1, -1, -1):
        n_copy(n).start()

    def m_recv(s):
        rc(MX.at[s], MX.at[s], m_s.at[0], m_r.at[s], me, ptn).wait_recv()

    for d in range(1, H):
        h2 = lax.rem(hi - d + H, H)
        m_recv(h2 * lo + low)
        for e in range(1, lo):
            m2_copy(e, h2).start()

    for k in range(1, Y):
        j = yk(k) * 2 + c
        rc(gn.at[j], gn.at[j], n2_s.at[k], n_r.at[j], me, ptn).wait_recv()
        n2_copy(k).start()
    for yy in range(Y):
        j = yy * 2 + oc
        rc(gn.at[j], gn.at[j], n_s.at[0], n_r.at[j], me, ptn).wait_recv()

    total = jnp.zeros((tok, 1), f32)
    inv = 1.0 / rm
    for j in range(T):
        cs = slice(j * col, (j + 1) * col)
        total = total + jnp.sum(
            (x_ref[:, cs].astype(f32) * inv) * (gain_ref[:, cs] * gn[j].astype(f32)), axis=1, keepdims=True
        )
    total = total * (1.0 / D)
    per = col // DB
    for j in range(T):
        cs = slice(j * col, (j + 1) * col)
        value = (
            cot_ref[:, cs].astype(f32)
            + (gain_ref[:, cs] * gn[j].astype(f32) - (x_ref[:, cs].astype(f32) * inv) * total) * inv
        ).astype(bf16)
        for q in range(per):
            gi[j * per + q] = value[:, q * DB:(q + 1) * DB].reshape(2, half, DB)

    def g_copy(i):
        s = dst_at(i)
        return rc(gi.at[s, c], GI.at[me, c], g_s.at[s], g_r.at[me], s, tp)

    def g2_copy(s):
        return rc(GI.at[s, c], GI.at[s, c], g2_s.at[s], g2_r.at[s], me, ptn)

    def issue_g(i, _):
        g_copy(i).start()
        return 0

    lax.fori_loop(1, G, issue_g, 0)

    loads[3].wait()

    acc = jnp.zeros((tok, ow.shape[1]), f32)
    for g in range(G):
        acc = acc + dot(gi[g].reshape(tok, DB), ow[g * DB:(g + 1) * DB, :])
    gm = acc.astype(bf16).astype(f32)
    gb_ref[...] = (gm * conv[...]).astype(bf16)
    gcv = gm * pb_ref[...].astype(f32)
    tail_s[...] = gcv[0:8]
    tail = rc(tail_s, tail_r, h_s.at[1], h_r.at[1], ring(me + G - 1), tp)
    tail.start()
    gmix[...] = gcv

    gow_ref[...] = dot(gi[me].reshape(tok, DB), MX[me], TN)

    for e in range(1, lo):
        lw = lax.rem(low + e, lo)
        for h2 in range(H):
            m_recv(h2 * lo + lw)

    tail.wait_recv()
    after = jnp.where(me < G - 1, tail_r[...], 0.0)
    pb2 = jnp.concatenate([gmix[...], after], axis=0)
    gp = taps_ref[2:3] * pb2[0:tok] + taps_ref[1:2] * pb2[1:1 + tok] + taps_ref[0:1] * pb2[2:2 + tok]
    gc_ref[...] = (gp * px_ref[...].astype(f32)).astype(bf16)
    gx_ref[...] = (gp * pc_ref[...].astype(f32)).astype(bf16)

    def finish(i, _):
        @pl.when(i < G)
        def _():
            s = src_at(i)
            rc(GI.at[s, c], GI.at[s, c], g_s.at[s], g_r.at[s], s, tp).wait_recv()
            g2_copy(s).start()

        @pl.when(i >= 2)
        def _():
            s = src_at(i - 1)
            rc(GI.at[s, oc], GI.at[s, oc], g2_s.at[s], g2_r.at[s], me, ptn).wait_recv()
            gow_ref[...] += dot(GI[s].reshape(tok, DB), MX[s], TN)

        return 0

    lax.fori_loop(1, G + 1, finish, 0)

    halo.wait_send()
    tail.wait_send()

    def drain(i, _):
        @pl.when(i > 0)
        def _():
            a_copy(i).wait_send()
            g_copy(i).wait_send()
            s = src_at(i)
            b_copy(s).wait_send()
            g2_copy(s).wait_send()

        s = src_at(i)
        for n in range(Y):
            fwd(n, s).wait_send()
        for k in range(1, Y):
            fwd2(k, s).wait_send()
            y_copy(k, s).wait_send()
        p_copy(s).wait_send()
        return 0

    lax.fori_loop(0, G, drain, 0)
    for d in range(1, H):
        m_copy(d).wait_send()
    for d in range(1, lo):
        for h2 in range(H):
            m2_copy(d, h2).wait_send()
    for n in range(Y):
        n_copy(n).wait_send()
    for k in range(1, Y):
        n2_copy(k).wait_send()
    for o in outs:
        o.wait()


def on_device(
    groups, slices,
    expert_input, norm_gain, expert_ids, route_weights, layer_cotangent,
    gate_weight, up_weight, down_weight, proj_b, proj_c, proj_x, conv_taps, out_weight,
):
    tok, D = expert_input.shape
    G, T = groups, slices
    Y = T // 2
    C = -(-(4 * tok // G) // 16) * 16
    lo = 1
    while lo * lo * 4 <= G:
        lo *= 2
    H = G // lo
    col = D // T
    DB = D // G
    F = gate_weight.shape[1]
    W = proj_b.shape[1]
    half = tok // 2
    vmem = pl.BlockSpec(memory_space=pltpu.VMEM)
    hbm = pl.BlockSpec(memory_space=pl.ANY)
    dma = pltpu.SemaphoreType.DMA
    V = pltpu.VMEM
    outs = pl.pallas_call(
        functools.partial(kernel, (G, T, C, lo)),
        out_shape=(
            jax.ShapeDtypeStruct((F, D), bf16),
            jax.ShapeDtypeStruct((F, D), bf16),
            jax.ShapeDtypeStruct((F, D), bf16),
            jax.ShapeDtypeStruct((DB, W), f32),
            jax.ShapeDtypeStruct((tok, W), bf16),
            jax.ShapeDtypeStruct((tok, W), bf16),
            jax.ShapeDtypeStruct((tok, W), bf16),
        ),
        in_specs=[vmem] * 5 + [hbm] * 3 + [vmem] * 4 + [hbm],
        out_specs=(hbm,) * 3 + (vmem,) * 4,
        scratch_shapes=[
            V((F, D), bf16), V((F, D), bf16), V((F, D), bf16), V((D, W), bf16),
            V((G * C, tok), bf16),
            V((G, 2, C, col), bf16),
            V((T, G, 2, C, col), bf16),
            V((G, C, F), bf16), V((G, C, F), bf16), V((G, C, F), bf16),
            V((G, Y, C, col), f32),
            V((G, Y, C, col), bf16), V((G, Y, C, col), bf16),
            V((G, Y, C, col), bf16), V((G, Y, C, col), bf16),
            V((G, C, col), bf16), V((G, C, col), bf16),
            V((T, tok, col), bf16),
            V((G, 2, half, DB), bf16), V((G, 2, half, DB), bf16),
            V((G, tok, W), bf16),
            V((tok, W), f32), V((tok, W), f32),
            V((8, W), f32), V((8, W), f32), V((8, W), f32), V((8, W), f32),
            V((F, D), bf16), V((F, D), bf16), V((F, D), bf16),
            dma((4,)), dma((3,)), dma(()),
            dma((G,)), dma((T, G)), dma((Y, G)), dma((Y, G)),
            dma((G,)), dma((G,)),
            dma((Y, G)), dma((Y, G)),
            dma((G,)), dma((G,)),
            dma((Y,)), dma((T,)), dma((Y,)),
            dma((H,)), dma((G,)), dma((lo, H)),
            dma((G,)), dma((G,)), dma((G,)), dma((G,)),
            dma((2,)), dma((2,)),
        ],
        compiler_params=pltpu.CompilerParams(
            collective_id=0, has_side_effects=True, vmem_limit_bytes=60 * 1024 * 1024
        ),
    )(
        expert_input, norm_gain[None, :], expert_ids.T, route_weights.T, layer_cotangent,
        gate_weight[0], up_weight[0], down_weight[0], proj_b, proj_c, proj_x, conv_taps, out_weight,
    )
    return (outs[0][None], outs[1][None], outs[2][None]) + tuple(outs[3:])


def solution(mesh):
    body = functools.partial(on_device, mesh.shape["sp"], mesh.shape["tp"])
    return jax.shard_map(
        body,
        mesh=mesh,
        in_specs=(
            P("sp", None), P(), P("sp", None), P("sp", None), P("sp", None),
            P("sp", "tp", None), P("sp", "tp", None), P("sp", "tp", None),
            P("sp", "tp"), P("sp", "tp"), P("sp", "tp"), P(None, "tp"), P(None, "tp"),
        ),
        out_specs=(
            P("sp", "tp", None), P("sp", "tp", None), P("sp", "tp", None),
            P("sp", "tp"), P("sp", "tp"), P("sp", "tp"), P("sp", "tp"),
        ),
        check_vma=False,
    )
```

```python
import functools

import jax
import jax.numpy as jnp
from jax import lax
from jax.experimental import pallas as pl
from jax.experimental.pallas import tpu as pltpu
from jax.sharding import PartitionSpec as P

eps = 1e-06
MESH = pl.DeviceIdType.MESH
f32 = jnp.float32
bf16 = jnp.bfloat16

NT = (((1,), (1,)), ((), ()))
TN = (((0,), (0,)), ((), ()))


def dot(a, b, dims=(((1,), (0,)), ((), ()))):
    return lax.dot_general(a, b, dims, preferred_element_type=f32)


def kernel(
    dims,
    x_ref, gain_ref, ids_ref, rw_ref, cot_ref, wg_h, wu_h, wd_h, pb_ref, pc_ref, px_ref, taps_ref, ow_h,
    gg_h, gu_h, gd_h, gow_ref, gb_ref, gc_ref, gx_ref,
    wg, wu, wd, ow, perm, send, R, hid, ggp, gup, pown, pcs, pcr, ysnd, yrcv, bsnd, back,
    gn, gi, GI, MX, conv, gmix, halo_s, halo_r, tail_s, tail_r, ggv, guv, gdv,
    lsem, osem, own_sem, a_s, r_sem, f_s, f2_s, p_s, p_r, y_s, y_r, b_s, b_r,
    n_s, n_r, n2_s, m_s, m_r, m2_s, g_s, g_r, g2_s, g2_r, h_s, h_r,
):
    G, T, C, lo = dims
    Y = T // 2
    H = G // lo
    tok, D = x_ref.shape
    col = D // T
    DB = D // G
    EARLY = min(2, H - 1)
    half = tok // 2
    me = lax.axis_index("sp")
    tp = lax.axis_index("tp")
    y = tp // 2
    c = lax.rem(tp, 2)
    oc = 1 - c
    ptn = y * 2 + oc

    def ring(v):
        return lax.rem(v + G, G)

    def yk(k):
        return lax.rem(y + k, Y)

    def rc(src, dst, ss, rs, sp, t):
        return pltpu.make_async_remote_copy(
            src_ref=src, dst_ref=dst, send_sem=ss, recv_sem=rs,
            device_id={"sp": sp, "tp": t}, device_id_type=MESH,
        )

    def far(i):
        k = i - 1
        d = G // 2 + ((k + 1) // 2) * (1 - 2 * lax.rem(k + 2, 2))
        return jnp.where(i == 0, 0, d)

    def src_at(i):
        return ring(me - far(i))

    def dst_at(i):
        return ring(me + far(i))

    loads = [
        pltpu.make_async_copy(h, v, lsem.at[n])
        for n, (h, v) in enumerate(((wg_h, wg), (wu_h, wu), (wd_h, wd), (ow_h, ow)))
    ]
    for ld in loads:
        ld.start()

    barrier = pltpu.get_barrier_semaphore()

    def greet(d, _):
        pl.semaphore_signal(barrier, inc=1, device_id={"sp": ring(me + d), "tp": tp}, device_id_type=MESH)
        return 0

    lax.fori_loop(1, G, greet, 0)
    for k in range(1, Y):
        pl.semaphore_signal(barrier, inc=1, device_id={"sp": me, "tp": yk(k) * 2 + c}, device_id_type=MESH)
    pl.semaphore_signal(barrier, inc=1, device_id={"sp": me, "tp": ptn}, device_id_type=MESH)

    xf = x_ref[...].astype(f32)
    rm = jnp.sqrt(jnp.mean(xf * xf, axis=1, keepdims=True) + eps)
    my_cols = pl.ds(pl.multiple_of(tp * col, col), col)
    ncols = ((x_ref[:, my_cols].astype(f32) / rm) * gain_ref[:, my_cols]).astype(bf16)
    ids = ids_ref[...]
    expert = lax.broadcasted_iota(jnp.int32, (G, tok), 0)
    is0 = expert == ids[0:1]
    is1 = expert == ids[1:2]
    both = jnp.where(is0 | is1, 1.0, 0.0).astype(bf16)
    earlier = jnp.where(
        lax.broadcasted_iota(jnp.int32, (tok, tok), 0) < lax.broadcasted_iota(jnp.int32, (tok, tok), 1), 1.0, 0.0
    ).astype(bf16)
    rank = dot(both, earlier)
    slot0 = jnp.sum(jnp.where(is0, rank, 0.0), axis=0, keepdims=True) + ids[0:1].astype(f32) * C
    slot1 = jnp.sum(jnp.where(is1, rank, 0.0), axis=0, keepdims=True) + ids[1:2].astype(f32) * C
    place = lax.broadcasted_iota(jnp.int32, (G * C, tok), 0).astype(f32)
    at0 = place == slot0
    at1 = place == slot1
    perm[...] = jnp.where(at0 | at1, 1.0, 0.0).astype(bf16)
    wslot = jnp.sum(jnp.where(at0, rw_ref[0:1], 0.0) + jnp.where(at1, rw_ref[1:2], 0.0), axis=1, keepdims=True)
    send[:, 0] = dot(perm[...], ncols).astype(bf16).reshape(G, C, col)
    send[:, 1] = (dot(perm[...], cot_ref[:, my_cols]) * wslot).astype(bf16).reshape(G, C, col)

    halo_s[...] = pc_ref[tok - 8:, :].astype(f32) * px_ref[tok - 8:, :].astype(f32)

    pl.semaphore_wait(barrier, G - 1 + Y)

    halo = rc(halo_s, halo_r, h_s.at[0], h_r.at[0], ring(me + 1), tp)
    halo.start()
    own = pltpu.make_async_copy(send.at[me], R.at[tp, me], own_sem)
    own.start()

    def a_copy(i):
        e = dst_at(i)
        return rc(send.at[e], R.at[tp, me], a_s.at[e], r_sem.at[tp, me], e, tp)

    def issue_a(i, _):
        a_copy(i).start()
        return 0

    lax.fori_loop(1, G, issue_a, 0)

    product = pc_ref[...].astype(f32) * px_ref[...].astype(f32)
    halo.wait_recv()
    before = jnp.where(me > 0, halo_r[...], 0.0)
    padded = jnp.concatenate([before, product], axis=0)
    cv = taps_ref[0:1] * padded[6:6 + tok] + taps_ref[1:2] * padded[7:7 + tok] + taps_ref[2:3] * product
    conv[...] = cv
    MX[me] = (pb_ref[...].astype(f32) * cv).astype(bf16)
    hi, low = me // lo, lax.rem(me, lo)

    def m_hop(h, way):
        s = h * lo + low
        to = lax.rem(hi + way + H, H)
        return rc(MX.at[s], MX.at[s], m_s.at[h, (way + 1) // 2], m_r.at[s], to * lo + low, tp)

    def m_start(h):
        @pl.when((h >= 0) & (h <= hi) & (hi < H - 1))
        def _():
            m_hop(h, 1).start()

        @pl.when((h < H) & (h >= hi) & (hi > 0))
        def _():
            m_hop(h, -1).start()

    def m_arrive(h):
        @pl.when((h >= 0) & (h < H))
        def _():
            m_recv(h * lo + low)
            m_start(h)
            for e in range(1, lo):
                m2_copy(e, h).start()

    def m_recv(s):
        rc(MX.at[s], MX.at[s], own_sem, m_r.at[s], me, ptn).wait_recv()

    m_start(hi)

    def m2_copy(d, h2):
        lw = lax.rem(low + d, lo)
        s = h2 * lo + low
        return rc(MX.at[s], MX.at[s], m2_s.at[d, h2], m_r.at[s], hi * lo + lw, tp)

    for d in range(1, lo):
        m2_copy(d, hi).start()

    for ld in loads[:3]:
        ld.wait()
    own.wait()

    def r_wait(j, s):
        rc(R.at[j, s], R.at[j, s], own_sem, r_sem.at[j, s], me, ptn).wait_recv()

    def fwd(n, s):
        t = ptn if n == 0 else yk(n) * 2 + c
        return rc(R.at[tp, s], R.at[tp, s], f_s.at[n, s], r_sem.at[tp, s], me, t)

    def fwd2(k, s):
        j = yk(k) * 2 + c
        return rc(R.at[j, s], R.at[j, s], f2_s.at[k, s], r_sem.at[j, s], me, ptn)

    def p_copy(s):
        return rc(pcs.at[s], pcr.at[s], p_s.at[s], p_r.at[s], me, ptn)

    def y_copy(k, s):
        yo = yk(k)
        return rc(ysnd.at[s, yo], yrcv.at[s, y], y_s.at[yo, s], y_r.at[y, s], me, yo * 2 + c)

    def b_copy(s):
        return rc(bsnd.at[s], back.at[me], b_s.at[s], b_r.at[me], s, tp)

    def cols(j):
        return pl.ds(pl.multiple_of(j * col, col), col)

    def step(i, _):
        for d in range(1, EARLY + 1):
            @pl.when(i == G + 2 * d - 2)
            def _():
                m_arrive(hi - d)
                m_arrive(hi + d)

        @pl.when(i < G)
        def _():
            s = src_at(i)

            @pl.when(i > 0)
            def _():
                r_wait(tp, s)

            for n in range(Y - 1, -1, -1):
                fwd(n, s).start()

        @pl.when((i >= 1) & (i < G + 1))
        def _():
            s = src_at(i - 1)
            for k in range(1, Y):
                r_wait(yk(k) * 2 + c, s)
                fwd2(k, s).start()

        @pl.when((i >= 2) & (i < G + 2))
        def _():
            s = src_at(i - 2)
            for yy in range(Y):
                r_wait(yy * 2 + oc, s)
            gate = jnp.zeros((C, wg.shape[0]), f32)
            up = gate
            gh = gate
            for j in range(T):
                rows = R[j, s, 0]
                cots = R[j, s, 1]
                cs = slice(j * col, (j + 1) * col)
                gate = gate + dot(rows, wg[:, cs], NT)
                up = up + dot(rows, wu[:, cs], NT)
                gh = gh + dot(cots, wd[:, cs], NT)
            sg = jax.nn.sigmoid(gate)
            hid[s] = (gate * sg * up).astype(bf16)
            a = (gh * up * sg * (1.0 + gate * (1.0 - sg))).astype(bf16)
            b = (gh * gate * sg).astype(bf16)
            ggp[s] = a
            gup[s] = b
            for yy in range(Y):
                jo = cols(yy * 2 + oc)
                pcs[s, yy] = (dot(a, wg[:, jo]) + dot(b, wu[:, jo])).astype(bf16)
            p_copy(s).start()
            for yy in range(Y):
                jm = cols(yy * 2 + c)
                pown[s, yy] = dot(a, wg[:, jm]) + dot(b, wu[:, jm])

        @pl.when((i >= 3) & (i < G + 3))
        def _():
            s = src_at(i - 3)
            p_copy(s).wait_recv()
            for k in range(1, Y):
                yo = yk(k)
                ysnd[s, yo] = (pown[s, yo] + pcr[s, yo].astype(f32)).astype(bf16)
                y_copy(k, s).start()

        @pl.when(i >= 4)
        def _():
            s = src_at(i - 4)
            total = pown[s, y] + pcr[s, y].astype(f32)
            for k in range(1, Y):
                yo = yk(k)
                rc(ysnd.at[s, yo], yrcv.at[s, yo], y_s.at[yo, s], y_r.at[yo, s], me, yo * 2 + c).wait_recv()
                total = total + yrcv[s, yo].astype(f32)

            @pl.when(i > 4)
            def _():
                bsnd[s] = total.astype(bf16)
                b_copy(s).start()

            @pl.when(i == 4)
            def _():
                back[me] = total.astype(bf16)

        return 0

    lax.fori_loop(0, G + 4, step, 0)

    def wgrad(j, _):
        rows = R[j, :, 0].reshape(G * C, col)
        cots = R[j, :, 1].reshape(G * C, col)
        F = wg.shape[0]
        gdv[:, cols(j)] = dot(hid[...].reshape(G * C, F), cots, TN).astype(bf16)
        ggv[:, cols(j)] = dot(ggp[...].reshape(G * C, F), rows, TN).astype(bf16)
        guv[:, cols(j)] = dot(gup[...].reshape(G * C, F), rows, TN).astype(bf16)
        return 0

    lax.fori_loop(0, T, wgrad, 0)
    outs = [
        pltpu.make_async_copy(v, h, osem.at[n]) for n, (v, h) in enumerate(((ggv, gg_h), (guv, gu_h), (gdv, gd_h)))
    ]
    for o in outs:
        o.start()

    for d in range(EARLY + 1, H):
        m_arrive(hi - d)
        m_arrive(hi + d)

    def back_wait(i, _):
        s = src_at(i)
        rc(back.at[s], back.at[s], b_s.at[s], b_r.at[s], s, tp).wait_recv()
        return 0

    lax.fori_loop(1, G, back_wait, 0)
    gn[tp] = dot(perm[...], back[...].reshape(G * C, col), TN).astype(bf16)

    def n_copy(n):
        t = ptn if n == 0 else yk(n) * 2 + c
        return rc(gn.at[tp], gn.at[tp], n_s.at[n], n_r.at[tp], me, t)

    def n2_copy(k):
        j = yk(k) * 2 + c
        return rc(gn.at[j], gn.at[j], n2_s.at[k], n_r.at[j], me, ptn)

    for n in range(Y - 1, -1, -1):
        n_copy(n).start()

    for k in range(1, Y):
        j = yk(k) * 2 + c
        rc(gn.at[j], gn.at[j], n2_s.at[k], n_r.at[j], me, ptn).wait_recv()
        n2_copy(k).start()
    for yy in range(Y):
        j = yy * 2 + oc
        rc(gn.at[j], gn.at[j], n_s.at[0], n_r.at[j], me, ptn).wait_recv()

    total = jnp.zeros((tok, 1), f32)
    inv = 1.0 / rm
    for j in range(T):
        cs = slice(j * col, (j + 1) * col)
        total = total + jnp.sum(
            (x_ref[:, cs].astype(f32) * inv) * (gain_ref[:, cs] * gn[j].astype(f32)), axis=1, keepdims=True
        )
    total = total * (1.0 / D)
    per = col // DB
    for j in range(T):
        cs = slice(j * col, (j + 1) * col)
        value = (
            cot_ref[:, cs].astype(f32)
            + (gain_ref[:, cs] * gn[j].astype(f32) - (x_ref[:, cs].astype(f32) * inv) * total) * inv
        ).astype(bf16)
        for q in range(per):
            gi[j * per + q] = value[:, q * DB:(q + 1) * DB].reshape(2, half, DB)

    def g_copy(i):
        s = dst_at(i)
        return rc(gi.at[s, c], GI.at[me, c], g_s.at[s], g_r.at[me], s, tp)

    def g2_copy(s):
        return rc(GI.at[s, c], GI.at[s, c], g2_s.at[s], g2_r.at[s], me, ptn)

    def issue_g(i, _):
        g_copy(i).start()
        return 0

    lax.fori_loop(1, G, issue_g, 0)

    loads[3].wait()

    acc = jnp.zeros((tok, ow.shape[1]), f32)
    for g in range(G):
        acc = acc + dot(gi[g].reshape(tok, DB), ow[g * DB:(g + 1) * DB, :])
    gm = acc.astype(bf16).astype(f32)
    gb_ref[...] = (gm * conv[...]).astype(bf16)
    gcv = gm * pb_ref[...].astype(f32)
    tail_s[...] = gcv[0:8]
    tail = rc(tail_s, tail_r, h_s.at[1], h_r.at[1], ring(me + G - 1), tp)
    tail.start()
    gmix[...] = gcv

    gow_ref[...] = dot(gi[me].reshape(tok, DB), MX[me], TN)

    for e in range(1, lo):
        lw = lax.rem(low + e, lo)
        for h2 in range(H):
            m_recv(h2 * lo + lw)

    tail.wait_recv()
    after = jnp.where(me < G - 1, tail_r[...], 0.0)
    pb2 = jnp.concatenate([gmix[...], after], axis=0)
    gp = taps_ref[2:3] * pb2[0:tok] + taps_ref[1:2] * pb2[1:1 + tok] + taps_ref[0:1] * pb2[2:2 + tok]
    gc_ref[...] = (gp * px_ref[...].astype(f32)).astype(bf16)
    gx_ref[...] = (gp * pc_ref[...].astype(f32)).astype(bf16)

    def finish(i, _):
        @pl.when(i < G)
        def _():
            s = src_at(i)
            rc(GI.at[s, c], GI.at[s, c], g_s.at[s], g_r.at[s], s, tp).wait_recv()
            g2_copy(s).start()

        @pl.when(i >= 2)
        def _():
            s = src_at(i - 1)
            rc(GI.at[s, oc], GI.at[s, oc], g2_s.at[s], g2_r.at[s], me, ptn).wait_recv()
            gow_ref[...] += dot(GI[s].reshape(tok, DB), MX[s], TN)

        return 0

    lax.fori_loop(1, G + 1, finish, 0)

    halo.wait_send()
    tail.wait_send()

    def drain(i, _):
        @pl.when(i > 0)
        def _():
            a_copy(i).wait_send()
            g_copy(i).wait_send()
            s = src_at(i)
            b_copy(s).wait_send()
            g2_copy(s).wait_send()

        s = src_at(i)
        for n in range(Y):
            fwd(n, s).wait_send()
        for k in range(1, Y):
            fwd2(k, s).wait_send()
            y_copy(k, s).wait_send()
        p_copy(s).wait_send()
        return 0

    lax.fori_loop(0, G, drain, 0)
    for h in range(H):
        @pl.when((h <= hi) & (hi < H - 1))
        def _():
            m_hop(h, 1).wait_send()

        @pl.when((h >= hi) & (hi > 0))
        def _():
            m_hop(h, -1).wait_send()

    for d in range(1, lo):
        for h2 in range(H):
            m2_copy(d, h2).wait_send()
    for n in range(Y):
        n_copy(n).wait_send()
    for k in range(1, Y):
        n2_copy(k).wait_send()
    for o in outs:
        o.wait()


PIECES = 2


def hand_over(*refs):
    srcs, dsts, bufs, (i_s, o_s) = refs[:7], refs[7:14], refs[14:21], refs[21:]
    ins, outs = [], []
    for n in range(7):
        rows = srcs[n].shape[0] // PIECES
        for p in range(PIECES):
            part = pl.ds(p * rows, rows)
            ins.append(pltpu.make_async_copy(srcs[n].at[part], bufs[n].at[part], i_s.at[n, p]))
            outs.append(pltpu.make_async_copy(bufs[n].at[part], dsts[n].at[part], o_s.at[n, p]))
    for a in ins:
        a.start()
    for a, o in zip(ins, outs):
        a.wait()
        o.start()
    for o in outs:
        o.wait()


def on_device(
    groups, slices,
    expert_input, norm_gain, expert_ids, route_weights, layer_cotangent,
    gate_weight, up_weight, down_weight, proj_b, proj_c, proj_x, conv_taps, out_weight,
):
    tok, D = expert_input.shape
    G, T = groups, slices
    Y = T // 2
    C = -(-(4 * tok // G) // 16) * 16
    lo = 1
    while lo * lo * 4 <= G:
        lo *= 2
    H = G // lo
    col = D // T
    DB = D // G
    F = gate_weight.shape[1]
    W = proj_b.shape[1]
    half = tok // 2
    vmem = pl.BlockSpec(memory_space=pltpu.VMEM)
    hbm = pl.BlockSpec(memory_space=pl.ANY)
    dma = pltpu.SemaphoreType.DMA
    V = pltpu.VMEM
    outs = pl.pallas_call(
        functools.partial(kernel, (G, T, C, lo)),
        out_shape=(
            jax.ShapeDtypeStruct((F, D), bf16),
            jax.ShapeDtypeStruct((F, D), bf16),
            jax.ShapeDtypeStruct((F, D), bf16),
            jax.ShapeDtypeStruct((DB, W), f32),
            jax.ShapeDtypeStruct((tok, W), bf16),
            jax.ShapeDtypeStruct((tok, W), bf16),
            jax.ShapeDtypeStruct((tok, W), bf16),
        ),
        in_specs=[vmem] * 5 + [hbm] * 3 + [vmem] * 4 + [hbm],
        out_specs=(hbm,) * 3 + (vmem,) * 4,
        scratch_shapes=[
            V((F, D), bf16), V((F, D), bf16), V((F, D), bf16), V((D, W), bf16),
            V((G * C, tok), bf16),
            V((G, 2, C, col), bf16),
            V((T, G, 2, C, col), bf16),
            V((G, C, F), bf16), V((G, C, F), bf16), V((G, C, F), bf16),
            V((G, Y, C, col), f32),
            V((G, Y, C, col), bf16), V((G, Y, C, col), bf16),
            V((G, Y, C, col), bf16), V((G, Y, C, col), bf16),
            V((G, C, col), bf16), V((G, C, col), bf16),
            V((T, tok, col), bf16),
            V((G, 2, half, DB), bf16), V((G, 2, half, DB), bf16),
            V((G, tok, W), bf16),
            V((tok, W), f32), V((tok, W), f32),
            V((8, W), f32), V((8, W), f32), V((8, W), f32), V((8, W), f32),
            V((F, D), bf16), V((F, D), bf16), V((F, D), bf16),
            dma((4,)), dma((3,)), dma(()),
            dma((G,)), dma((T, G)), dma((Y, G)), dma((Y, G)),
            dma((G,)), dma((G,)),
            dma((Y, G)), dma((Y, G)),
            dma((G,)), dma((G,)),
            dma((Y,)), dma((T,)), dma((Y,)),
            dma((H, 2)), dma((G,)), dma((lo, H)),
            dma((G,)), dma((G,)), dma((G,)), dma((G,)),
            dma((2,)), dma((2,)),
        ],
        compiler_params=pltpu.CompilerParams(
            collective_id=0, has_side_effects=True, vmem_limit_bytes=60 * 1024 * 1024
        ),
    )(
        expert_input, norm_gain[None, :], expert_ids.T, route_weights.T, layer_cotangent,
        gate_weight[0], up_weight[0], down_weight[0], proj_b, proj_c, proj_x, conv_taps, out_weight,
    )
    return (outs[0][None], outs[1][None], outs[2][None]) + tuple(outs[3:])


def solution(mesh):
    body = functools.partial(on_device, mesh.shape["sp"], mesh.shape["tp"])
    return jax.shard_map(
        body,
        mesh=mesh,
        in_specs=(
            P("sp", None), P(), P("sp", None), P("sp", None), P("sp", None),
            P("sp", "tp", None), P("sp", "tp", None), P("sp", "tp", None),
            P("sp", "tp"), P("sp", "tp"), P("sp", "tp"), P(None, "tp"), P(None, "tp"),
        ),
        out_specs=(
            P("sp", "tp", None), P("sp", "tp", None), P("sp", "tp", None),
            P("sp", "tp"), P("sp", "tp"), P("sp", "tp"), P("sp", "tp"),
        ),
        check_vma=False,
    )
```
